128 devices in a mesh: dp: 4 (over x), kv: 16 (over z, y), tp: 2 (over core).
Axes of the slice: x: 4, y: 4, z: 4, core: 2. Of those that a mesh axis runs over, the one named last changes fastest.
Arguments:
- tokens: bfloat16 [8192, 2048], P('dp', 'kv'), may hold values from -70 to 70
- pre_gain: float32 [2048], replicated, may hold values from 0.1 to 1.9
- query_weight: bfloat16 [2048, 1024], P(None, 'tp'), may hold values from -0.125 to 0.125
- key_weight: bfloat16 [2048, 1024], P(None, 'tp'), may hold values from -0.125 to 0.125
- value_weight: bfloat16 [2048, 1024], P(None, 'tp'), may hold values from -0.125 to 0.125
- gate_weight: bfloat16 [2048, 1024], P(None, 'tp'), may hold values from -0.125 to 0.125
- beta_weight: bfloat16 [2048, 8], replicated, may hold values from -0.125 to 0.125
- decay_weight: bfloat16 [2048, 8], replicated, may hold values from -0.125 to 0.125
- decay_log: float32 [8], P('tp'), may hold values from -3 to 0.5
- head_gain: float32 [128], replicated, may hold values from 0.1 to 1.9
- out_weight: bfloat16 [1024, 2048], P('tp', 'kv'), may hold values from -1 to 1
- post_gain: float32 [2048], P(('kv', 'tp')), may hold values from 0.1 to 1.9
- saved_state: float32 [2048, 8, 128, 128], P(('dp', 'kv'), 'tp'), may hold values from -4 to 4
- earlier_keys: bfloat16 [2048, 4, 8, 128], P(('dp', 'kv'), None, 'tp'), may hold values from -6 to 6
- earlier_values: bfloat16 [2048, 4, 8, 128], P(('dp', 'kv'), None, 'tp'), may hold values from -6 to 6
- earlier_rates: float32 [2048, 4, 8], P(('dp', 'kv'), None, 'tp'), may hold values from 0.05 to 0.95
- earlier_decays: float32 [2048, 4, 8], P(('dp', 'kv'), None, 'tp'), may hold values from -1.5 to -0.02
- accepted: int32 [2048], P(('dp', 'kv')), may hold values from 0 to 4
Outputs:
- mixed: bfloat16 [8192, 2048], P('dp', ('kv', 'tp'))
- committed: float32 [2048, 8, 128, 128], P(('dp', 'kv'), 'tp')
The draws below stay inside these ranges and needn't reach their ends.
All inputs are finite; a program needn't handle non-finite values.
Results may differ from the reference program's by a relative error of at most 0.011.
Values may be sent and summed in bfloat16 or wider, within the bound.
No kernel may reach another device: no remote copies, remote signals or barrier semaphores. Data moves between devices by JAX's collectives and lax.ppermute only.
A program may use at most 128 MiB of HBM per device.

```python
import jax
import jax.numpy as jnp
from jax import lax

D = 2048
HEADS = 8
HEAD = 128
PROPOSALS = 4
SEQS = 2048
ROWS = 8192


def draw_tokens(key, part):
    columns = jnp.arange(D, dtype=jnp.float32)
    rising = 1.0 + 3.0 * columns / D
    base = jnp.clip(jax.random.normal(key, (ROWS, D), jnp.float32), -5.0, 5.0)
    return (base * rising).astype(jnp.bfloat16)


def draw_out_weight(key, part):
    columns = jnp.arange(D, dtype=jnp.float32)
    rising = (1.0 + 3.0 * columns / D) * (HEADS * HEAD) ** (-0.5)
    base = jnp.clip(jax.random.normal(key, (HEADS * HEAD, D), jnp.float32), -6.0, 6.0)
    return jnp.clip(base * rising, -1.0, 1.0).astype(jnp.bfloat16)


def place_ends(entries, stream_key, smallest, top_value):
    dims = entries.shape
    spot = [jax.random.randint(jax.random.fold_in(stream_key, axis), (), 0, dims[axis]) for axis in range(len(dims))]
    entries = entries.at[tuple(spot)].set(smallest)
    longest = dims.index(max(dims))
    spot[longest] = (spot[longest] + 1) % dims[longest]
    return entries.at[tuple(spot)].set(top_value)


def level_of(key, extent, cuts, least, high):
    def one(dim, shards_of):
        heights = jax.random.uniform(jax.random.fold_in(jax.random.fold_in(key, 6), dim), (shards_of,), jnp.float32, least / len(cuts), high / len(cuts))
        return jnp.repeat(jnp.exp(heights), extent[dim] // shards_of).reshape((-1,) + (1,) * (len(extent) - dim - 1))

    loudness = one(*cuts[0])
    for cut in cuts[1:]:
        loudness = loudness * one(*cut)
    return loudness


def normal_values(rng, extent, deviation, most, cuts=(), kind=jnp.bfloat16):
    values = deviation * jax.random.normal(rng, extent, jnp.float32)
    if cuts:
        values = values * level_of(rng, extent, cuts, -0.22, 0.18)
    return jnp.clip(values, -most, most).astype(kind)


def setup_inputs(seed: int = 0) -> dict:
    splits = jax.random.split(jax.random.key(seed), 19)
    return {
        "tokens": draw_tokens(jax.random.fold_in(splits[18], 71), 0),
        "pre_gain": jnp.clip(1.0 + 0.18 * jax.random.normal(splits[1], (D,), jnp.float32), 0.1, 1.9),
        "query_weight": normal_values(splits[2], (D, HEADS * HEAD), D ** -0.5, 0.125, ((1, 2),)),
        "key_weight": normal_values(splits[3], (D, HEADS * HEAD), D ** -0.5, 0.125, ((1, 2),)),
        "value_weight": normal_values(splits[4], (D, HEADS * HEAD), D ** -0.5, 0.125, ((1, 2),)),
        "gate_weight": normal_values(splits[5], (D, HEADS * HEAD), D ** -0.5, 0.125, ((1, 2),)),
        "beta_weight": normal_values(splits[6], (D, HEADS), D ** -0.5, 0.125),
        "decay_weight": normal_values(splits[7], (D, HEADS), D ** -0.5, 0.125),
        "decay_log": jnp.clip(-3.0 + 3.5 * jax.random.uniform(splits[8], (HEADS,), jnp.float32) ** level_of(splits[8], (HEADS,), ((0, 2),), -0.2, 0.2), -3.0, 0.5),
        "head_gain": jnp.clip(1.0 + 0.18 * jax.random.normal(splits[9], (HEAD,), jnp.float32), 0.1, 1.9),
        "out_weight": draw_out_weight(jax.random.fold_in(splits[18], 71), 0),
        "post_gain": jnp.clip(1.0 + 0.18 * jax.random.normal(splits[11], (D,), jnp.float32), 0.1, 1.9),
        "saved_state": normal_values(splits[12], (SEQS, HEADS, HEAD, HEAD), 0.3, 4.0, ((0, 64), (1, 2)), jnp.float32),
        "earlier_keys": normal_values(splits[13], (SEQS, PROPOSALS, HEADS, HEAD), 1.0, 6.0, ((0, 64), (2, 2))),
        "earlier_values": normal_values(splits[14], (SEQS, PROPOSALS, HEADS, HEAD), 1.0, 6.0, ((0, 64), (2, 2))),
        "earlier_rates": jnp.clip(0.05 + 0.9 * jax.random.uniform(splits[15], (SEQS, PROPOSALS, HEADS), jnp.float32) ** level_of(splits[15], (SEQS, PROPOSALS, HEADS), ((0, 64), (2, 2)), -0.2, 0.2), 0.05, 0.95),
        "earlier_decays": jnp.clip(-1.5 + 1.48 * jax.random.uniform(splits[16], (SEQS, PROPOSALS, HEADS), jnp.float32) ** level_of(splits[16], (SEQS, PROPOSALS, HEADS), ((0, 64), (2, 2)), -0.2, 0.2), -1.5, -0.02),
        "accepted": place_ends(jax.random.randint(splits[17], (SEQS,), 0, PROPOSALS + 1), jax.random.fold_in(splits[17], 1), 0, PROPOSALS).astype(jnp.int32),
    }


def unit_norm(values):
    return values * lax.rsqrt(lax.optimization_barrier(jnp.sum(values * values, axis=-1, keepdims=True)) + 1e-06)

def advance(current, key_row, value_row, rate_now, log_decay):
    recalled = lax.optimization_barrier(jnp.sum(key_row[..., :, None] * current, axis=-2))
    rate_cube = rate_now[..., None, None]
    current = current - rate_cube * key_row[..., :, None] * recalled[..., None, :]
    return jnp.exp(log_decay)[..., None, None] * current + rate_cube * key_row[..., :, None] * value_row[..., None, :]

def run_heads(saved_state, earlier_keys, earlier_values, earlier_rates, earlier_decays, accepted, queries, keys_unit, values_act, rates, decays):
    current = saved_state
    proposals = earlier_keys.shape[1]
    for position in range(proposals):
        live = (position < accepted).astype(jnp.float32)
        live = live.reshape(live.shape + (1,) * (earlier_rates.ndim - 2))
        current = advance(current, earlier_keys[:, position], earlier_values[:, position], earlier_rates[:, position] * live, earlier_decays[:, position] * live)
    committed = current
    outputs = []
    for position in range(proposals):
        current = advance(current, keys_unit[:, position], values_act[:, position], rates[:, position], decays[:, position])
        outputs.append(lax.optimization_barrier(jnp.sum(queries[:, position][..., :, None] * current, axis=-2)))
    return (committed, jnp.stack(outputs, axis=1))

def reference(tokens, pre_gain, query_weight, key_weight, value_weight, gate_weight, beta_weight, decay_weight, decay_log, head_gain, out_weight, post_gain, saved_state, earlier_keys, earlier_values, earlier_rates, earlier_decays, accepted):
    widened = tokens.astype(jnp.float32)
    inverse = lax.rsqrt(lax.optimization_barrier(jnp.mean(widened * widened, axis=1, keepdims=True)) + 1e-06)
    scaled = (widened * pre_gain).astype(jnp.bfloat16)

    def project(weight):
        return jnp.dot(scaled, weight, preferred_element_type=jnp.float32) * inverse

    def heads_of(values):
        return values.reshape(SEQS, PROPOSALS, HEADS, HEAD)
    queries = unit_norm(jax.nn.silu(heads_of(project(query_weight)))) * HEAD ** (-0.5)
    keys_unit = unit_norm(jax.nn.silu(heads_of(project(key_weight))))
    values_act = jax.nn.silu(heads_of(project(value_weight)))
    gates_raw = heads_of(project(gate_weight))
    rates = jax.nn.sigmoid(project(beta_weight)).reshape(SEQS, PROPOSALS, HEADS)
    decays = -jnp.exp(decay_log) * jax.nn.softplus(project(decay_weight)).reshape(SEQS, PROPOSALS, HEADS)
    earlier_unit = unit_norm(earlier_keys.astype(jnp.float32))
    earlier_vals = earlier_values.astype(jnp.float32)

    def per_head(items):
        return run_heads(items[0], items[1], items[2], items[3], items[4], accepted, items[5], items[6], items[7], items[8], items[9])
    items = (jnp.moveaxis(saved_state, 1, 0), jnp.moveaxis(earlier_unit, 2, 0), jnp.moveaxis(earlier_vals, 2, 0), jnp.moveaxis(earlier_rates, 2, 0), jnp.moveaxis(earlier_decays, 2, 0), jnp.moveaxis(queries, 2, 0), jnp.moveaxis(keys_unit, 2, 0), jnp.moveaxis(values_act, 2, 0), jnp.moveaxis(rates, 2, 0), jnp.moveaxis(decays, 2, 0))
    committed, reads = lax.map(per_head, items)
    committed = jnp.moveaxis(committed, 0, 1)
    reads = jnp.moveaxis(reads, 0, 2)
    normed = reads * lax.rsqrt(lax.optimization_barrier(jnp.mean(reads * reads, axis=-1, keepdims=True)) + 1e-06) * head_gain
    attended = (normed * jax.nn.silu(gates_raw)).reshape(ROWS, HEADS * HEAD).astype(jnp.bfloat16)
    projected = jnp.dot(attended, out_weight, preferred_element_type=jnp.float32)
    factor = lax.rsqrt(lax.optimization_barrier(jnp.mean(projected * projected, axis=1, keepdims=True)) + 1e-06)
    mixed = (projected * factor * post_gain).astype(jnp.bfloat16)
    return (mixed, committed)
```

```python
import functools
import jax
import jax.numpy as jnp
from jax import lax
from jax.experimental import pallas as pl
from jax.experimental.pallas import tpu as pltpu
from jax.sharding import PartitionSpec as P

F32 = jnp.float32
BF16 = jnp.bfloat16
EPS = 1e-06


def dot(a, b):
    return jnp.dot(a.astype(BF16), b.astype(BF16), preferred_element_type=F32)


def dot_t(a, b):
    return lax.dot_general(
        a.astype(BF16), b.astype(BF16), (((1,), (1,)), ((), ())), preferred_element_type=F32
    )


def unit(values):
    return values * lax.rsqrt(jnp.sum(values * values, axis=-1, keepdims=True) + EPS)


def silu(values):
    return values / (1.0 + jnp.exp(-values))


def chain_terms(log_decays, steps):
    rows = log_decays.shape[0]
    place = lax.broadcasted_iota(jnp.int32, log_decays.shape, 0) % steps
    total = log_decays
    shift = 1
    while shift < steps:
        total = total + jnp.where(place >= shift, pltpu.roll(total, shift, 0), 0.0)
        shift *= 2
    rest = jnp.where(place + 1 < steps, pltpu.roll(log_decays, rows - 1, 0), 0.0)
    shift = 1
    while shift < steps:
        rest = rest + jnp.where(place + shift < steps, pltpu.roll(rest, rows - shift, 0), 0.0)
        shift *= 2
    return total, rest


def chain_writes(keys, values, recalled, rates, total, steps):
    rows = keys.shape[0]
    row = lax.broadcasted_iota(jnp.int32, (rows, rows), 0)
    col = lax.broadcasted_iota(jnp.int32, (rows, rows), 1)
    same = row // steps == col // steps
    before = same & (col < row)
    gaps = total[:, :rows] - total[:, :rows].T
    fade = jnp.exp(jnp.where(same & (col <= row), gaps, 0.0))
    mix = jnp.where(before, rates * fade * dot_t(keys, keys), 0.0)
    start = rates * (values - jnp.exp(total[:, : values.shape[1]]) * recalled)
    done = start
    once = dot(mix, start)
    twice = dot(mix, once)
    done = start + twice
    done = done - dot(mix, done)
    return done, fade, same & (col <= row)


def by_sequence(left, states, steps):
    rows = left[0].shape[0]
    tile = 8
    per = tile // steps
    outs = [[] for _ in left]
    for first in range(0, rows, tile):
        stack = jnp.concatenate([part[first : first + tile] for part in left], axis=0)
        held = jnp.concatenate([states(first // steps + i) for i in range(per)], axis=1)
        size = held.shape[1] // per
        got = dot(stack, held)
        for index in range(len(left)):
            piece = got[index * tile : (index + 1) * tile]
            which = lax.broadcasted_iota(jnp.int32, (tile, size), 0) // steps
            value = piece[:, :size]
            for i in range(1, per):
                value = jnp.where(which == i, piece[:, i * size : (i + 1) * size], value)
            outs[index].append(value)
    return [jnp.concatenate(part, axis=0) for part in outs]


def commit_kernel(steps, state_ref, keys_ref, values_ref, coef_ref, out_ref):
    seqs, heads, size, _ = state_ref.shape
    span = seqs * steps
    rows = span * heads

    def stack(ref):
        return jnp.concatenate(
            [ref[:, h * size : (h + 1) * size].astype(F32) for h in range(heads)], axis=0
        )

    def column(first):
        return jnp.concatenate(
            [
                jnp.broadcast_to(coef_ref[:, first + h : first + h + 1], (span, size))
                for h in range(heads)
            ],
            axis=0,
        )

    keys = unit(stack(keys_ref))
    values = stack(values_ref)
    rates = column(0)
    total, rest = chain_terms(column(heads), steps)

    def state_of(index):
        return state_ref[index % seqs, index // seqs].astype(BF16)

    (recalled,) = by_sequence([keys], state_of, steps)
    writes, _, _ = chain_writes(keys, values, recalled, rates, total, steps)
    writes = jnp.exp(rest) * writes
    whole = jnp.exp(total + rest)
    keys_t = keys.T.astype(BF16)
    group = lax.broadcasted_iota(jnp.int32, (rows, size), 0) // steps
    for index in range(0, seqs * heads, 2):
        pair = jnp.concatenate(
            [jnp.where(group == index + i, writes, 0.0).astype(BF16) for i in range(2)], axis=1
        )
        added = jnp.dot(keys_t, pair, preferred_element_type=F32)
        for i in range(2):
            s, h = (index + i) % seqs, (index + i) // seqs
            scale = whole[(index + i) * steps : (index + i) * steps + 1]
            out_ref[s, h] = scale * state_ref[s, h] + added[:, i * size : (i + 1) * size]


def commit(saved_state, keys, values, coef, steps):
    seqs, heads, size, _ = saved_state.shape
    block = 8
    span = block * steps
    return pl.pallas_call(
        functools.partial(commit_kernel, steps),
        grid=(seqs // block,),
        out_shape=jax.ShapeDtypeStruct(saved_state.shape, F32),
        in_specs=[
            pl.BlockSpec((block, heads, size, size), lambda i: (i, 0, 0, 0)),
            pl.BlockSpec((span, heads * size), lambda i: (i, 0)),
            pl.BlockSpec((span, heads * size), lambda i: (i, 0)),
            pl.BlockSpec((span, coef.shape[1]), lambda i: (i, 0)),
        ],
        out_specs=pl.BlockSpec((block, heads, size, size), lambda i: (i, 0, 0, 0)),
        name="commit",
    )(saved_state, keys, values, coef)


def read_kernel(
    steps,
    tokens_ref,
    gain_ref,
    query_ref,
    key_ref,
    value_ref,
    gate_ref,
    small_ref,
    log_ref,
    head_gain_ref,
    state_ref,
    out_ref,
    scaled_ref,
    inverse_ref,
    coef_ref,
):
    head = pl.program_id(0)
    blocks, rows, width = tokens_ref.shape
    size = state_ref.shape[2]
    heads = log_ref.shape[1]

    @pl.when(head == 0)
    def _():
        squares = jnp.zeros((rows, width), F32)
        for j in range(blocks):
            wide = tokens_ref[j].astype(F32)
            squares = squares + wide * wide
            scaled_ref[:, j * width : (j + 1) * width] = (wide * gain_ref[j : j + 1]).astype(BF16)
        mean = jnp.sum(squares, axis=1, keepdims=True) / (blocks * width)
        inverse = lax.rsqrt(mean + EPS)
        inverse_ref[...] = jnp.broadcast_to(inverse, inverse_ref.shape)
        raw = jnp.dot(scaled_ref[...], small_ref[...], preferred_element_type=F32) * inverse
        rates = 1.0 / (1.0 + jnp.exp(-raw[:, :heads]))
        lift = raw[:, heads:]
        soft = jnp.maximum(lift, 0.0) + jnp.log1p(jnp.exp(-jnp.abs(lift)))
        coef_ref[:, :heads] = rates
        coef_ref[:, heads : 2 * heads] = -jnp.exp(log_ref[...]) * soft

    scaled = scaled_ref[...]
    inverse = inverse_ref[...]

    def project(ref):
        return jnp.dot(scaled, ref[...], preferred_element_type=F32) * inverse

    lane = lax.broadcasted_iota(jnp.int32, (rows, 2 * heads), 1)

    def column(index):
        picked = jnp.sum(jnp.where(lane == index, coef_ref[...], 0.0), axis=1, keepdims=True)
        return jnp.broadcast_to(picked, (rows, size))

    queries = unit(silu(project(query_ref))) * size ** (-0.5)
    keys = unit(silu(project(key_ref)))
    values = silu(project(value_ref))
    gates = silu(project(gate_ref))
    rates = column(head)
    total, _ = chain_terms(column(head + heads), steps)

    def state_of(index):
        return state_ref[index, 0].astype(BF16)

    recalled, seen = by_sequence([keys, queries], state_of, steps)
    writes, fade, upto = chain_writes(keys, values, recalled, rates, total, steps)
    weights = jnp.where(upto, fade * dot_t(queries, keys), 0.0)
    reads = jnp.exp(total) * seen + dot(weights, writes)
    mean = jnp.sum(reads * reads, axis=1, keepdims=True) / size
    out_ref[...] = (reads * lax.rsqrt(mean + EPS) * head_gain_ref[...] * gates).astype(BF16)


def read(tokens, gain, weights, small, decay_log, head_gain, committed, steps):
    blocks, rows, width = tokens.shape
    seqs, heads, size, _ = committed.shape
    model = blocks * width
    whole = lambda *shape: pl.BlockSpec(shape, lambda i: (0,) * len(shape))
    return pl.pallas_call(
        functools.partial(read_kernel, steps),
        grid=(heads,),
        out_shape=jax.ShapeDtypeStruct((rows, heads * size), BF16),
        in_specs=[
            whole(blocks, rows, width),
            whole(blocks, width),
            *[pl.BlockSpec((model, size), lambda i: (0, i)) for _ in range(4)],
            whole(model, 2 * heads),
            whole(1, heads),
            whole(1, size),
            pl.BlockSpec((seqs, 1, size, size), lambda i: (0, i, 0, 0)),
        ],
        out_specs=pl.BlockSpec((rows, size), lambda i: (0, i)),
        scratch_shapes=[
            pltpu.VMEM((rows, model), BF16),
            pltpu.VMEM((rows, size), F32),
            pltpu.VMEM((rows, 2 * heads), F32),
        ],
        name="read",
    )(tokens, gain, *weights, small, decay_log, head_gain, committed)


def project_kernel(left_ref, right_ref, weight_ref, out_ref, square_ref):
    blocks, depth, width = weight_ref.shape
    half = width // 2
    rows = left_ref.shape[0]
    left = left_ref[...]
    right = right_ref[...]
    squares = jnp.zeros((rows, half), F32)
    for j in range(blocks):
        both = weight_ref[j]
        first = jnp.dot(left, both, preferred_element_type=F32)
        second = jnp.dot(right, both, preferred_element_type=F32)
        value = first[:, :half] + second[:, half:]
        squares = squares + value * value
        out_ref[j] = value
    total = jnp.sum(squares, axis=1, keepdims=True)
    square_ref[...] = jnp.broadcast_to(total, square_ref.shape)


def project(left, right, weight):
    blocks, depth, width = weight.shape
    rows = left.shape[0]
    return pl.pallas_call(
        project_kernel,
        out_shape=(
            jax.ShapeDtypeStruct((blocks, rows, width // 2), F32),
            jax.ShapeDtypeStruct((rows, 128), F32),
        ),
        name="project",
    )(left, right, weight)


def normalize_kernel(model, value_ref, mine_ref, other_ref, out_ref):
    blocks, rows, half = value_ref.shape
    total = mine_ref[:, :half] + other_ref[:, :half]
    factor = lax.rsqrt(total / model + EPS)
    for j in range(blocks):
        value = value_ref[j] * factor
        out_ref[j] = jnp.concatenate([value[: rows // 2], value[rows // 2 :]], axis=1).astype(BF16)


def normalize(value, mine, other, model):
    blocks, rows, half = value.shape
    return pl.pallas_call(
        functools.partial(normalize_kernel, model),
        out_shape=jax.ShapeDtypeStruct((blocks, rows // 2, 2 * half), BF16),
        name="normalize",
    )(value, mine, other)


def spread_kernel(value_ref, gain_ref, out_ref):
    blocks, rows, width = value_ref.shape
    half = width // 2
    gain = gain_ref[...]
    for j in range(blocks):
        value = value_ref[j].astype(F32)
        base = 2 * rows * j
        out_ref[base : base + rows] = (value[:, :half] * gain).astype(BF16)
        out_ref[base + rows : base + 2 * rows] = (value[:, half:] * gain).astype(BF16)


def spread(value, gain):
    blocks, rows, width = value.shape
    return pl.pallas_call(
        spread_kernel,
        out_shape=jax.ShapeDtypeStruct((blocks * rows * 2, width // 2), BF16),
        name="spread",
    )(value, gain)


def local(
    tokens,
    pre_gain,
    query_weight,
    key_weight,
    value_weight,
    gate_weight,
    beta_weight,
    decay_weight,
    decay_log,
    head_gain,
    out_weight,
    post_gain,
    saved_state,
    earlier_keys,
    earlier_values,
    earlier_rates,
    earlier_decays,
    accepted,
):
    seqs, heads, size, _ = saved_state.shape
    steps = earlier_keys.shape[1]
    rows = seqs * steps
    model = pre_gain.shape[0]
    groups = lax.axis_size("kv")
    core = lax.axis_index("tp")
    swap = [(0, 1), (1, 0)]

    own = lax.all_to_all(
        tokens.reshape(groups, rows, tokens.shape[1]), "kv", 0, 0, tiled=True
    )
    depth, cols = out_weight.shape
    half = cols // 2
    keep = lax.dynamic_slice_in_dim(out_weight, core * half, half, 1)
    give = lax.dynamic_slice_in_dim(out_weight, (1 - core) * half, half, 1)
    got = lax.ppermute(give, "tp", swap)
    both = jnp.concatenate([keep, got], axis=1)
    wide = lax.all_to_all(
        jnp.broadcast_to(both[None], (groups, depth, cols)), "kv", 0, 0, tiled=True
    )

    live = jnp.arange(steps)[None, :, None] < accepted[:, None, None]
    coef = jnp.concatenate(
        [jnp.where(live, earlier_rates, 0.0), jnp.where(live, earlier_decays, 0.0)], axis=2
    ).reshape(rows, 2 * heads)
    committed = commit(
        saved_state,
        earlier_keys.reshape(rows, heads * size),
        earlier_values.reshape(rows, heads * size),
        coef,
        steps,
    )
    small = jnp.concatenate(
        [
            lax.dynamic_slice_in_dim(weight, core * heads, heads, 1)
            for weight in (beta_weight, decay_weight)
        ],
        axis=1,
    )
    attended = read(
        own,
        pre_gain.reshape(groups, -1),
        (query_weight, key_weight, value_weight, gate_weight),
        small,
        decay_log.reshape(1, heads),
        head_gain.reshape(1, size),
        committed,
        steps,
    )
    other = lax.ppermute(attended, "tp", swap)
    value, mine = project(attended, other, wide)
    theirs = lax.ppermute(mine, "tp", swap)
    packed = normalize(value, mine, theirs, model)
    arrived = lax.all_to_all(packed, "kv", 0, 0, tiled=True)
    mixed = spread(arrived, post_gain.reshape(1, half))
    return (mixed, committed)


def solution(mesh):
    placed = (
        P("dp", "kv"),
        P(),
        P(None, "tp"),
        P(None, "tp"),
        P(None, "tp"),
        P(None, "tp"),
        P(),
        P(),
        P("tp"),
        P(),
        P("tp", "kv"),
        P(("kv", "tp")),
        P(("dp", "kv"), "tp", None, None),
        P(("dp", "kv"), None, "tp", None),
        P(("dp", "kv"), None, "tp", None),
        P(("dp", "kv"), None, "tp"),
        P(("dp", "kv"), None, "tp"),
        P(("dp", "kv")),
    )
    return jax.shard_map(
        local,
        mesh=mesh,
        in_specs=placed,
        out_specs=(P("dp", ("kv", "tp")), P(("dp", "kv"), "tp", None, None)),
        check_vma=False,
    )
```

```python
import functools
import jax
import jax.numpy as jnp
from jax import lax
from jax.experimental import pallas as pl
from jax.experimental.pallas import tpu as pltpu
from jax.sharding import PartitionSpec as P

F32 = jnp.float32
BF16 = jnp.bfloat16
EPS = 1e-06
AHEAD = 4
READ_AHEAD = 6
CUTS = 2
Y = 4
TEAM = 2
VMEM = pltpu.VMEM
WHOLE = pl.BlockSpec(memory_space=pltpu.VMEM)
FAR = pl.BlockSpec(memory_space=pltpu.HBM)
SCALAR = pl.BlockSpec(memory_space=pltpu.SMEM)


def params(mib):
    return pltpu.CompilerParams(vmem_limit_bytes=mib * 1024 * 1024)


def near(value):
    return pltpu.with_memory_space_constraint(value, pltpu.VMEM)


def far(value):
    return pltpu.with_memory_space_constraint(value, pltpu.HBM)


def dot(a, b):
    return jnp.dot(a.astype(BF16), b.astype(BF16), preferred_element_type=F32)


def dot_t(a, b):
    return lax.dot_general(
        a.astype(BF16), b.astype(BF16), (((1,), (1,)), ((), ())), preferred_element_type=F32
    )


def unit(values):
    return values * lax.rsqrt(jnp.sum(values * values, axis=-1, keepdims=True) + EPS)


def silu(values):
    return values / (1.0 + jnp.exp(-values))


def chain_terms(log_decays, steps):
    rows = log_decays.shape[0]
    place = lax.broadcasted_iota(jnp.int32, log_decays.shape, 0) % steps
    total = log_decays
    shift = 1
    while shift < steps:
        total = total + jnp.where(place >= shift, pltpu.roll(total, shift, 0), 0.0)
        shift *= 2
    rest = jnp.where(place + 1 < steps, pltpu.roll(log_decays, rows - 1, 0), 0.0)
    shift = 1
    while shift < steps:
        rest = rest + jnp.where(place + shift < steps, pltpu.roll(rest, rows - shift, 0), 0.0)
        shift *= 2
    return total, rest


def chain_mix(keys, rates, total, steps):
    rows = keys.shape[0]
    row = lax.broadcasted_iota(jnp.int32, (rows, rows), 0)
    col = lax.broadcasted_iota(jnp.int32, (rows, rows), 1)
    upto = (row // steps == col // steps) & (col <= row)
    fade = jnp.exp(jnp.where(upto, total - total.T, 0.0))
    mix = jnp.where(upto & (col < row), rates * fade * dot_t(keys, keys), 0.0)
    return mix.astype(BF16), jnp.where(upto, fade, 0.0)


def chain_writes(mix, start):
    done = start + dot(mix, dot(mix, start))
    return done - dot(mix, done)


def by_sequence(left, states, steps):
    rows = left[0].shape[0]
    tile = 8
    per = tile // steps
    outs = [[] for _ in left]
    for first in range(0, rows, tile):
        stack = jnp.concatenate([part[first : first + tile] for part in left], axis=0)
        held = jnp.concatenate([states(first // steps + i) for i in range(per)], axis=1)
        size = held.shape[1] // per
        got = dot(stack, held)
        which = lax.broadcasted_iota(jnp.int32, (tile, size), 0) // steps
        for index in range(len(left)):
            piece = got[index * tile : (index + 1) * tile]
            value = piece[:, :size]
            for i in range(1, per):
                value = jnp.where(which == i, piece[:, i * size : (i + 1) * size], value)
            outs[index].append(value)
    return [jnp.concatenate(part, axis=0) for part in outs]


def recall_kernel(
    steps,
    source_ref,
    keys_ref,
    values_ref,
    coef_ref,
    state_ref,
    unit_ref,
    writes_ref,
    whole_ref,
    held_ref,
    short_ref,
    in_sems,
    out_sems,
):
    heads, seqs, size, _ = held_ref.shape
    rows = seqs * steps
    arrive = [
        pltpu.make_async_copy(source_ref.at[:, h], held_ref.at[h], in_sems.at[h])
        for h in range(heads)
    ]
    leave = [
        pltpu.make_async_copy(short_ref.at[h], state_ref.at[h], out_sems.at[h])
        for h in range(heads)
    ]
    for copy in arrive[:AHEAD]:
        copy.start()
    ready = []
    for h in range(heads):
        lanes = slice(h * size, (h + 1) * size)
        keys = unit(keys_ref[:, lanes].astype(F32))
        rates = jnp.broadcast_to(coef_ref[:, h : h + 1], (rows, size))
        total, rest = chain_terms(
            jnp.broadcast_to(coef_ref[:, heads + h : heads + h + 1], (rows, size)), steps
        )
        mix, _ = chain_mix(keys, rates, total, steps)
        unit_ref[:, lanes] = keys.astype(BF16)
        whole_ref[:, lanes] = jnp.exp(total + rest)
        given = rates * values_ref[:, lanes].astype(F32)
        ready.append((keys, mix, given, rates * jnp.exp(total), jnp.exp(rest)))
    starts = []
    for h in range(heads):
        keys, mix, given, scale, _ = ready[h]
        arrive[h].wait()
        if h + AHEAD < heads:
            arrive[h + AHEAD].start()
        short_ref[h] = held_ref[h].astype(BF16)
        leave[h].start()
        (recalled,) = by_sequence([keys], lambda s: short_ref[h, s], steps)
        starts.append(given - scale * recalled)
    for h in range(heads):
        lanes = slice(h * size, (h + 1) * size)
        writes_ref[:, lanes] = (ready[h][4] * chain_writes(ready[h][1], starts[h])).astype(BF16)
    for copy in leave:
        copy.wait()


def recall(state, keys, values, coef, steps):
    rows, width = keys.shape
    seqs, heads, size, _ = state.shape
    turned = (heads, seqs, size, size)
    return pl.pallas_call(
        functools.partial(recall_kernel, steps),
        out_shape=(
            pltpu.HBM(turned, BF16),
            VMEM((rows, width), BF16),
            VMEM((rows, width), BF16),
            VMEM((rows, width), F32),
        ),
        in_specs=[FAR] + [WHOLE] * 3,
        out_specs=(FAR,) + (WHOLE,) * 3,
        scratch_shapes=[
            pltpu.VMEM(turned, F32),
            pltpu.VMEM(turned, BF16),
            pltpu.SemaphoreType.DMA((heads,)),
            pltpu.SemaphoreType.DMA((heads,)),
        ],
        compiler_params=params(20),
        name="recall",
    )(state, keys, values, coef)


COMMIT_BLOCK = 4
COMMIT_AHEAD = 3


def commit_kernel(steps, state_ref, unit_ref, writes_ref, whole_ref, out_ref, held_ref, ins, outs):
    seqs, heads, size, _ = held_ref.shape
    span = COMMIT_BLOCK * steps

    def part(ref, step):
        return ref.at[pl.ds(step * COMMIT_BLOCK, COMMIT_BLOCK)]

    def arrive(step):
        return pltpu.make_async_copy(part(state_ref, step), part(held_ref, step), ins.at[step])

    def leave(step):
        return pltpu.make_async_copy(part(held_ref, step), part(out_ref, step), outs.at[step])

    count = seqs // COMMIT_BLOCK
    for step in range(COMMIT_AHEAD):
        arrive(step).start()
    group = lax.broadcasted_iota(jnp.int32, (span, size), 0) // steps

    def body(step, carry):
        base = pl.multiple_of(step * span, span)
        arrive(step).wait()

        @pl.when(step + COMMIT_AHEAD < count)
        def _():
            arrive(step + COMMIT_AHEAD).start()

        for h in range(heads):
            lanes = slice(h * size, (h + 1) * size)
            keys_t = unit_ref[pl.ds(base, span), lanes].astype(F32).T.astype(BF16)
            writes = writes_ref[pl.ds(base, span), lanes].astype(F32)
            whole = whole_ref[pl.ds(base, span), lanes]
            for s in range(0, COMMIT_BLOCK, 2):
                pair = jnp.concatenate(
                    [jnp.where(group == s + i, writes, 0.0).astype(BF16) for i in range(2)], axis=1
                )
                added = jnp.dot(keys_t, pair, preferred_element_type=F32)
                for i in range(2):
                    scale = whole[(s + i) * steps : (s + i) * steps + 1]
                    at = step * COMMIT_BLOCK + s + i
                    held_ref[at, h] = scale * held_ref[at, h] + added[:, i * size : (i + 1) * size]
        leave(step).start()
        return carry

    lax.fori_loop(0, count, body, 0)
    for step in range(count):
        leave(step).wait()


def commit(state, keys, writes, whole, steps):
    count = state.shape[0] // COMMIT_BLOCK
    return pl.pallas_call(
        functools.partial(commit_kernel, steps),
        out_shape=pltpu.HBM(state.shape, F32),
        in_specs=[FAR] + [WHOLE] * 3,
        out_specs=FAR,
        scratch_shapes=[
            pltpu.VMEM(state.shape, F32),
            pltpu.SemaphoreType.DMA((count,)),
            pltpu.SemaphoreType.DMA((count,)),
        ],
        compiler_params=params(16),
        cost_estimate=pl.CostEstimate(flops=4 * 10**9, bytes_accessed=0, transcendentals=0),
        name="commit",
    )(state, keys, writes, whole)


def read_kernel(
    steps,
    core_ref,
    tokens_ref,
    gain_ref,
    query_ref,
    key_ref,
    value_ref,
    gate_ref,
    beta_ref,
    decay_ref,
    log_ref,
    head_gain_ref,
    state_ref,
    unit_ref,
    writes_ref,
    whole_ref,
    out_ref,
    scaled_ref,
    held_ref,
    near_ref,
    sems,
    state_sems,
):
    blocks, rows, width = tokens_ref.shape
    heads, _, size, _ = state_ref.shape
    part = blocks * width // CUTS
    copies = [
        [
            pltpu.make_async_copy(
                ref.at[pl.ds(c * part, part)],
                held_ref.at[i, pl.ds(c * part, part)],
                sems.at[i * CUTS + c],
            )
            for c in range(CUTS)
        ]
        for i, ref in enumerate((query_ref, key_ref, value_ref, gate_ref))
    ]
    states = [
        pltpu.make_async_copy(state_ref.at[h], near_ref.at[h], state_sems.at[h])
        for h in range(heads)
    ]
    queue = [*copies[1], *copies[0], *states, *copies[2], *copies[3]]
    for copy in queue[:READ_AHEAD]:
        copy.start()
    taken = [0]

    def arrive(count):
        for index in range(taken[0], taken[0] + count):
            queue[index].wait()
            if index + READ_AHEAD < len(queue):
                queue[index + READ_AHEAD].start()
        taken[0] += count

    squares = jnp.zeros((rows, width), F32)
    for j in range(blocks):
        wide = tokens_ref[j].astype(F32)
        squares = squares + wide * wide
        scaled_ref[:, j * width : (j + 1) * width] = (wide * gain_ref[j : j + 1]).astype(BF16)
    mean = jnp.sum(squares, axis=1, keepdims=True) / (blocks * width)
    inverse = lax.rsqrt(mean + EPS)
    scaled = scaled_ref[...]
    small = jnp.concatenate([beta_ref[...], decay_ref[...]], axis=0)
    raw = dot_t(scaled, small) * inverse
    every = beta_ref.shape[0]
    lane = lax.broadcasted_iota(jnp.int32, raw.shape, 1)
    first = core_ref[0] * heads

    def column(index):
        picked = jnp.sum(jnp.where(lane == first + index, raw, 0.0), axis=1, keepdims=True)
        return jnp.broadcast_to(picked, (rows, size))

    def project(index):
        raw = jnp.dot(scaled, held_ref[index], preferred_element_type=F32) * inverse
        return [raw[:, h * size : (h + 1) * size] for h in range(heads)]

    row = lax.broadcasted_iota(jnp.int32, (rows, rows), 0)
    col = lax.broadcasted_iota(jnp.int32, (rows, rows), 1)
    same = row // steps == col // steps
    all_heads = range(heads)
    lanes = [slice(h * size, (h + 1) * size) for h in all_heads]
    rates, totals = [], []
    for h in all_heads:
        rates.append(1.0 / (1.0 + jnp.exp(-column(h))))
        lift = column(every + h)
        soft = jnp.maximum(lift, 0.0) + jnp.log1p(jnp.exp(-jnp.abs(lift)))
        totals.append(chain_terms(-jnp.exp(log_ref[:, h : h + 1]) * soft, steps)[0])
    arrive(CUTS)
    keys = [unit(silu(raw)) for raw in project(1)]
    mixes, fades = zip(*(chain_mix(keys[h], rates[h], totals[h], steps) for h in all_heads))
    arrive(CUTS)
    queries = [unit(silu(raw)) * size ** (-0.5) for raw in project(0)]
    weights = [fades[h] * dot_t(queries[h], keys[h]) for h in all_heads]

    def caught_up(left, h):
        recent = jnp.where(same, dot_t(left, unit_ref[:, lanes[h]]), 0.0)
        return dot(recent, writes_ref[:, lanes[h]])

    recents = [(caught_up(keys[h], h), caught_up(queries[h], h)) for h in all_heads]
    arrive(heads)
    recalls, seens = [], []
    for h in all_heads:
        recalled, seen = by_sequence([keys[h], queries[h]], lambda s: near_ref[h, s], steps)
        whole = whole_ref[:, lanes[h]]
        decay = jnp.exp(totals[h])
        recalls.append(rates[h] * decay * (whole * recalled + recents[h][0]))
        seens.append(decay * (whole * seen + recents[h][1]))
    arrive(CUTS)
    reads = []
    for h, raw in enumerate(project(2)):
        writes = chain_writes(mixes[h], rates[h] * silu(raw) - recalls[h])
        value = seens[h] + dot(weights[h], writes)
        mean = jnp.sum(value * value, axis=1, keepdims=True) / size
        reads.append(value * lax.rsqrt(mean + EPS) * head_gain_ref[...])
    arrive(CUTS)
    for h, raw in enumerate(project(3)):
        out_ref[:, lanes[h]] = (reads[h] * silu(raw)).astype(BF16)


def read(core, tokens, gain, weights, beta, decay, decay_log, head_gain, state, kept, steps):
    blocks, rows, width = tokens.shape
    heads, _, size, _ = state.shape
    return pl.pallas_call(
        functools.partial(read_kernel, steps),
        out_shape=VMEM((rows, heads * size), BF16),
        in_specs=[SCALAR] + [WHOLE] * 2 + [FAR] * 4 + [WHOLE] * 4 + [FAR] + [WHOLE] * 3,
        out_specs=WHOLE,
        scratch_shapes=[
            pltpu.VMEM((rows, blocks * width), BF16),
            pltpu.VMEM((4, blocks * width, heads * size), BF16),
            pltpu.VMEM(state.shape, BF16),
            pltpu.SemaphoreType.DMA((4 * CUTS,)),
            pltpu.SemaphoreType.DMA((heads,)),
        ],
        compiler_params=params(24),
        name="read",
    )(core, tokens, gain, *weights, beta, decay, decay_log, head_gain, state, *kept)


def project_kernel(team, *refs):
    *weight_refs, full_ref, send_ref = refs[team:]
    rows = jnp.concatenate([ref[...] for ref in refs[:team]], axis=0)
    for a in range(team):
        for y in range(Y):
            value = dot_t(weight_refs[y][a], rows)
            full_ref[a * Y + y] = value
            send_ref[a * Y + y] = value.astype(BF16)


def project(parts, weights):
    pairs, cols, _ = weights[0].shape
    shape = (pairs * len(weights), cols, len(parts) * parts[0].shape[0])
    return pl.pallas_call(
        functools.partial(project_kernel, len(parts)),
        out_shape=(VMEM(shape, F32), VMEM(shape, BF16)),
        in_specs=[WHOLE] * (len(parts) + len(weights)),
        out_specs=(WHOLE,) * 2,
        compiler_params=params(8),
        name="project",
    )(*parts, *weights)


def combine_kernel(core_ref, mine_ref, other_ref, sum_ref, square_ref):
    blocks, cols, rows = mine_ref.shape
    half = cols // 2
    squares = jnp.zeros((8, rows), F32)
    for j in range(blocks):
        value = mine_ref[j] + other_ref[j].astype(F32)
        squares = squares + jnp.sum((value * value).reshape(cols // 8, 8, rows), axis=0)
    square_ref[...] = squares
    own = pl.ds(pl.multiple_of(core_ref[0] * half, half), half)
    for j in range(blocks):
        sum_ref[j] = mine_ref[j, own, :] + other_ref[j, own, :].astype(F32)


def combine(core, mine, other):
    blocks, cols, rows = mine.shape
    return pl.pallas_call(
        combine_kernel,
        out_shape=(VMEM((blocks, cols // 2, rows), F32), VMEM((8, rows), F32)),
        in_specs=[SCALAR, WHOLE, WHOLE],
        out_specs=(WHOLE,) * 2,
        compiler_params=params(8),
        name="combine",
    )(core, mine, other)


def normalize_kernel(team, model, place_ref, sum_ref, *refs):
    out_ref = refs[team]
    blocks, _, rows = sum_ref.shape
    span = rows // team
    factors = []
    for e in range(team):
        total = 0.0
        for f in range(team):
            part = refs[f][:, (e ^ f) * span : ((e ^ f) + 1) * span]
            total = total + jnp.sum(part, axis=0, keepdims=True)
        factors.append(lax.rsqrt(total / model + EPS))
    factor = jnp.concatenate(factors, axis=1)
    for j in range(blocks):
        out_ref[jnp.bitwise_xor(place_ref[0], j)] = (sum_ref[j] * factor).astype(BF16)


def normalize(place, sums, squares, model):
    return pl.pallas_call(
        functools.partial(normalize_kernel, len(squares), model),
        out_shape=VMEM(sums.shape, BF16),
        in_specs=[SCALAR] + [WHOLE] * (1 + len(squares)),
        out_specs=WHOLE,
        compiler_params=params(8),
        name="normalize",
    )(place, sums, *squares)


def spread_kernel(team, depth_ref, value_ref, gain_ref, out_ref):
    blocks, _, rows = value_ref.shape
    span = rows // team
    gain = gain_ref[...]
    depth = depth_ref[0]
    for m in range(blocks):
        sender = (m // Y) * team + depth % team if team < Y else depth
        value = value_ref[m].astype(F32) * gain
        for e in range(team):
            source = jnp.bitwise_xor(sender, e) * Y + m % Y
            lanes = pl.ds(pl.multiple_of(source * span, span), span)
            out_ref[:, lanes] = value[:, e * span : (e + 1) * span].astype(BF16)


def spread(depth, value, gain, team):
    blocks, cols, rows = value.shape
    return pl.pallas_call(
        functools.partial(spread_kernel, team),
        out_shape=jax.ShapeDtypeStruct((cols, blocks * rows), BF16),
        in_specs=[SCALAR, WHOLE, WHOLE],
        compiler_params=params(8),
        name="spread",
    )(depth, value, gain)


def layer(
    tokens,
    pre_gain,
    query_weight,
    key_weight,
    value_weight,
    gate_weight,
    beta_weight,
    decay_weight,
    decay_log,
    head_gain,
    out_weight,
    post_gain,
    saved_state,
    earlier_keys,
    earlier_values,
    earlier_rates,
    earlier_decays,
    accepted,
):
    seqs, heads, size, _ = saved_state.shape
    steps = earlier_keys.shape[1]
    rows = seqs * steps
    model = pre_gain.shape[0]
    groups = lax.axis_size("kv")
    deep = groups // Y
    core = lax.axis_index("tp").reshape(1)
    depth = (lax.axis_index("kv") // Y).reshape(1)
    place = (depth // TEAM) * Y + lax.axis_index("kv") % Y
    swap = [(0, 1), (1, 0)]
    members = [
        [z * Y + y for z in range(first, deep, TEAM) for y in range(Y)] for first in range(TEAM)
    ]

    def shift(value, mask):
        return lax.ppermute(value, "kv", [(k, k ^ mask) for k in range(groups)])

    flipped = out_weight.T
    across = shift(flipped, TEAM * Y)
    own = lax.all_to_all(
        tokens.reshape(groups, rows, tokens.shape[1]), "kv", 0, 0, tiled=True
    )
    two = jnp.stack([flipped, across])
    wide = []
    for y in range(1, Y):
        wide.append(near(shift(two, y)))
    live = jnp.arange(steps)[None, :, None] < accepted[:, None, None]
    coef = jnp.concatenate(
        [jnp.where(live, earlier_rates, 0.0), jnp.where(live, earlier_decays, 0.0)], axis=2
    ).reshape(rows, 2 * heads)
    state, *kept = recall(
        far(saved_state),
        near(earlier_keys.reshape(rows, heads * size)),
        near(earlier_values.reshape(rows, heads * size)),
        near(coef),
        steps,
    )
    state = far(state)
    kept = tuple(near(value) for value in kept)
    attended = read(
        core,
        near(own),
        near(pre_gain.reshape(groups, -1)),
        tuple(far(w) for w in (query_weight, key_weight, value_weight, gate_weight)),
        near(beta_weight.T),
        near(decay_weight.T),
        near(decay_log.reshape(1, heads)),
        near(head_gain.reshape(1, size)),
        state,
        kept,
        steps,
    )
    parts = [attended] + [shift(attended, e * Y) for e in range(1, TEAM)]
    full, send = project([near(part) for part in parts], [near(two), *wide])
    other = lax.ppermute(send, "tp", swap)
    sums, squares = combine(core, near(full), near(other))
    squares = [squares] + [shift(squares, e * Y) for e in range(1, TEAM)]
    packed = normalize(place, near(sums), [near(part) for part in squares], model)
    arrived = lax.all_to_all(packed, "kv", 0, 0, axis_index_groups=members, tiled=True)
    committed = commit(far(saved_state), *kept, steps)
    mixed = spread(depth, near(arrived), near(post_gain.reshape(-1, 1)), TEAM).T
    return (mixed, committed)


def solution(mesh):
    placed = (
        P("dp", "kv"),
        P(),
        P(None, "tp"),
        P(None, "tp"),
        P(None, "tp"),
        P(None, "tp"),
        P(),
        P(),
        P("tp"),
        P(),
        P("tp", "kv"),
        P(("kv", "tp")),
        P(("dp", "kv"), "tp", None, None),
        P(("dp", "kv"), None, "tp", None),
        P(("dp", "kv"), None, "tp", None),
        P(("dp", "kv"), None, "tp"),
        P(("dp", "kv"), None, "tp"),
        P(("dp", "kv")),
    )
    return jax.shard_map(
        layer,
        mesh=mesh,
        in_specs=placed,
        out_specs=(P("dp", ("kv", "tp")), P(("dp", "kv"), "tp", None, None)),
        check_vma=False,
    )
```

```python
import functools
import jax
import jax.numpy as jnp
from jax import lax
from jax.experimental import pallas as pl
from jax.experimental.pallas import tpu as pltpu
from jax.sharding import PartitionSpec as P

F32 = jnp.float32
BF16 = jnp.bfloat16
EPS = 1e-06
AHEAD = 4
READ_AHEAD = 6
CUTS = 2
Y = 4
TEAM = 2
VMEM = pltpu.VMEM
WHOLE = pl.BlockSpec(memory_space=pltpu.VMEM)
FAR = pl.BlockSpec(memory_space=pltpu.HBM)
SCALAR = pl.BlockSpec(memory_space=pltpu.SMEM)


def params(mib):
    return pltpu.CompilerParams(vmem_limit_bytes=mib * 1024 * 1024)


def near(value):
    return pltpu.with_memory_space_constraint(value, pltpu.VMEM)


def far(value):
    return pltpu.with_memory_space_constraint(value, pltpu.HBM)


def dot(a, b):
    return jnp.dot(a.astype(BF16), b.astype(BF16), preferred_element_type=F32)


def dot_t(a, b):
    return lax.dot_general(
        a.astype(BF16), b.astype(BF16), (((1,), (1,)), ((), ())), preferred_element_type=F32
    )


def unit(values):
    return values * lax.rsqrt(jnp.sum(values * values, axis=-1, keepdims=True) + EPS)


def silu(values):
    return values / (1.0 + jnp.exp(-values))


def chain_terms(log_decays, steps):
    rows = log_decays.shape[0]
    place = lax.broadcasted_iota(jnp.int32, log_decays.shape, 0) % steps
    total = log_decays
    shift = 1
    while shift < steps:
        total = total + jnp.where(place >= shift, pltpu.roll(total, shift, 0), 0.0)
        shift *= 2
    rest = jnp.where(place + 1 < steps, pltpu.roll(log_decays, rows - 1, 0), 0.0)
    shift = 1
    while shift < steps:
        rest = rest + jnp.where(place + shift < steps, pltpu.roll(rest, rows - shift, 0), 0.0)
        shift *= 2
    return total, rest


def chain_mix(keys, rates, total, steps):
    rows = keys.shape[0]
    row = lax.broadcasted_iota(jnp.int32, (rows, rows), 0)
    col = lax.broadcasted_iota(jnp.int32, (rows, rows), 1)
    upto = (row // steps == col // steps) & (col <= row)
    fade = jnp.exp(jnp.where(upto, total - total.T, 0.0))
    mix = jnp.where(upto & (col < row), rates * fade * dot_t(keys, keys), 0.0)
    return mix.astype(BF16), jnp.where(upto, fade, 0.0)


def chain_writes(mix, start):
    done = start + dot(mix, dot(mix, start))
    return done - dot(mix, done)


def by_sequence(left, states, steps):
    rows = left[0].shape[0]
    tile = 8
    per = tile // steps
    outs = [[] for _ in left]
    for first in range(0, rows, tile):
        stack = jnp.concatenate([part[first : first + tile] for part in left], axis=0)
        held = jnp.concatenate([states(first // steps + i) for i in range(per)], axis=1)
        size = held.shape[1] // per
        got = dot(stack, held)
        which = lax.broadcasted_iota(jnp.int32, (tile, size), 0) // steps
        for index in range(len(left)):
            piece = got[index * tile : (index + 1) * tile]
            value = piece[:, :size]
            for i in range(1, per):
                value = jnp.where(which == i, piece[:, i * size : (i + 1) * size], value)
            outs[index].append(value)
    return [jnp.concatenate(part, axis=0) for part in outs]


def recall_kernel(
    steps,
    source_ref,
    keys_ref,
    values_ref,
    rates_ref,
    decays_ref,
    accepted_ref,
    state_ref,
    unit_ref,
    writes_ref,
    whole_ref,
    held_ref,
    short_ref,
    flat_ref,
    given_ref,
    chain_ref,
    count_ref,
    small_sems,
    in_sems,
    out_sems,
):
    heads, seqs, size, _ = held_ref.shape
    rows = seqs * steps
    arrive = [
        pltpu.make_async_copy(source_ref.at[:, h], held_ref.at[h], in_sems.at[h])
        for h in range(heads)
    ]
    leave = [
        pltpu.make_async_copy(short_ref.at[h], state_ref.at[h], out_sems.at[h])
        for h in range(heads)
    ]
    small = [
        pltpu.make_async_copy(keys_ref, given_ref.at[0], small_sems.at[0]),
        pltpu.make_async_copy(values_ref, given_ref.at[1], small_sems.at[1]),
        pltpu.make_async_copy(rates_ref, chain_ref.at[0], small_sems.at[2]),
        pltpu.make_async_copy(decays_ref, chain_ref.at[1], small_sems.at[3]),
        pltpu.make_async_copy(accepted_ref, count_ref, small_sems.at[4]),
    ]
    for copy in small + arrive[:AHEAD]:
        copy.start()
    for copy in small:
        copy.wait()
    table = jnp.concatenate(
        [chain_ref[i, p] for i in range(2) for p in range(steps)]
        + [jnp.broadcast_to(count_ref[...].astype(F32), (8, seqs))],
        axis=0,
    )
    pick = (
        lax.broadcasted_iota(jnp.int32, (rows, seqs), 0) // steps
        == lax.broadcasted_iota(jnp.int32, (rows, seqs), 1)
    ).astype(F32)
    spread = lax.dot_general(
        pick,
        table,
        (((1,), (1,)), ((), ())),
        precision=lax.Precision.HIGHEST,
        preferred_element_type=F32,
    )
    lane = lax.broadcasted_iota(jnp.int32, spread.shape, 1)
    place = lax.broadcasted_iota(jnp.int32, spread.shape, 0) % steps
    count = steps * heads

    def column(index):
        picked = jnp.sum(jnp.where(lane == index, spread, 0.0), axis=1, keepdims=True)
        return jnp.broadcast_to(picked, (rows, size))

    live = column(2 * count) > place[:, :1].astype(F32)

    def own(first):
        return jnp.where(live, column(first + place * heads), 0.0)

    for i in range(2):
        flat_ref[i] = given_ref[i].astype(F32).reshape(rows * heads, size)
    ready = []
    for h in range(heads):
        lanes = slice(h * size, (h + 1) * size)
        keys = unit(flat_ref[0, pl.ds(h, rows, heads), :])
        rates = own(h)
        total, rest = chain_terms(own(count + h), steps)
        mix, _ = chain_mix(keys, rates, total, steps)
        unit_ref[:, lanes] = keys.astype(BF16)
        whole_ref[:, lanes] = jnp.exp(total + rest)
        given = rates * flat_ref[1, pl.ds(h, rows, heads), :]
        ready.append((keys, mix, given, rates * jnp.exp(total), jnp.exp(rest)))
    starts = []
    for h in range(heads):
        keys, mix, given, scale, _ = ready[h]
        arrive[h].wait()
        if h + AHEAD < heads:
            arrive[h + AHEAD].start()
        short_ref[h] = held_ref[h].astype(BF16)
        leave[h].start()
        (recalled,) = by_sequence([keys], lambda s: short_ref[h, s], steps)
        starts.append(given - scale * recalled)
    for h in range(heads):
        lanes = slice(h * size, (h + 1) * size)
        writes_ref[:, lanes] = (ready[h][4] * chain_writes(ready[h][1], starts[h])).astype(BF16)
    for copy in leave:
        copy.wait()


def recall(state, keys, values, rates, decays, accepted, steps):
    seqs, heads, size, _ = state.shape
    rows, width = seqs * steps, heads * size
    turned = (heads, seqs, size, size)
    return pl.pallas_call(
        functools.partial(recall_kernel, steps),
        out_shape=(
            pltpu.HBM(turned, BF16),
            VMEM((rows, width), BF16),
            VMEM((rows, width), BF16),
            VMEM((rows, width), F32),
        ),
        in_specs=[FAR] * 6,
        out_specs=(FAR,) + (WHOLE,) * 3,
        scratch_shapes=[
            pltpu.VMEM(turned, F32),
            pltpu.VMEM(turned, BF16),
            pltpu.VMEM((2, rows * heads, size), F32),
            pltpu.VMEM((2, *keys.shape), BF16),
            pltpu.VMEM((2, *rates.shape), F32),
            pltpu.VMEM(accepted.shape, jnp.int32),
            pltpu.SemaphoreType.DMA((5,)),
            pltpu.SemaphoreType.DMA((heads,)),
            pltpu.SemaphoreType.DMA((heads,)),
        ],
        compiler_params=params(20),
        name="recall",
    )(state, keys, values, rates, decays, accepted)


COMMIT_BLOCK = 4
COMMIT_AHEAD = 3


def commit_kernel(steps, state_ref, unit_ref, writes_ref, whole_ref, out_ref, held_ref, ins, outs):
    seqs, heads, size, _ = held_ref.shape
    span = COMMIT_BLOCK * steps

    def part(ref, step):
        return ref.at[pl.ds(step * COMMIT_BLOCK, COMMIT_BLOCK)]

    def arrive(step):
        return pltpu.make_async_copy(part(state_ref, step), part(held_ref, step), ins.at[step])

    def leave(step):
        return pltpu.make_async_copy(part(held_ref, step), part(out_ref, step), outs.at[step])

    count = seqs // COMMIT_BLOCK
    for step in range(COMMIT_AHEAD):
        arrive(step).start()
    group = lax.broadcasted_iota(jnp.int32, (span, size), 0) // steps

    def body(step, carry):
        base = pl.multiple_of(step * span, span)
        arrive(step).wait()

        @pl.when(step + COMMIT_AHEAD < count)
        def _():
            arrive(step + COMMIT_AHEAD).start()

        for h in range(heads):
            lanes = slice(h * size, (h + 1) * size)
            keys_t = unit_ref[pl.ds(base, span), lanes].astype(F32).T.astype(BF16)
            writes = writes_ref[pl.ds(base, span), lanes].astype(F32)
            whole = whole_ref[pl.ds(base, span), lanes]
            for s in range(0, COMMIT_BLOCK, 2):
                pair = jnp.concatenate(
                    [jnp.where(group == s + i, writes, 0.0).astype(BF16) for i in range(2)], axis=1
                )
                added = jnp.dot(keys_t, pair, preferred_element_type=F32)
                for i in range(2):
                    scale = whole[(s + i) * steps : (s + i) * steps + 1]
                    at = step * COMMIT_BLOCK + s + i
                    held_ref[at, h] = scale * held_ref[at, h] + added[:, i * size : (i + 1) * size]
        leave(step).start()
        return carry

    lax.fori_loop(0, count, body, 0)
    for step in range(count):
        leave(step).wait()


def commit(state, keys, writes, whole, steps):
    count = state.shape[0] // COMMIT_BLOCK
    return pl.pallas_call(
        functools.partial(commit_kernel, steps),
        out_shape=pltpu.HBM(state.shape, F32),
        in_specs=[FAR] + [WHOLE] * 3,
        out_specs=FAR,
        scratch_shapes=[
            pltpu.VMEM(state.shape, F32),
            pltpu.SemaphoreType.DMA((count,)),
            pltpu.SemaphoreType.DMA((count,)),
        ],
        compiler_params=params(16),
        cost_estimate=pl.CostEstimate(flops=4 * 10**9, bytes_accessed=0, transcendentals=0),
        name="commit",
    )(state, keys, writes, whole)


def read_kernel(
    steps,
    core_ref,
    tokens_ref,
    gain_ref,
    query_ref,
    key_ref,
    value_ref,
    gate_ref,
    beta_ref,
    decay_ref,
    log_ref,
    head_gain_ref,
    state_ref,
    unit_ref,
    writes_ref,
    whole_ref,
    out_ref,
    scaled_ref,
    held_ref,
    near_ref,
    sems,
    state_sems,
):
    blocks, rows, width = tokens_ref.shape
    heads, _, size, _ = state_ref.shape
    part = blocks * width // CUTS
    copies = [
        [
            pltpu.make_async_copy(
                ref.at[pl.ds(c * part, part)],
                held_ref.at[i, pl.ds(c * part, part)],
                sems.at[i * CUTS + c],
            )
            for c in range(CUTS)
        ]
        for i, ref in enumerate((query_ref, key_ref, value_ref, gate_ref))
    ]
    states = [
        pltpu.make_async_copy(state_ref.at[h], near_ref.at[h], state_sems.at[h])
        for h in range(heads)
    ]
    queue = [*copies[1], *copies[0], *states, *copies[2], *copies[3]]
    for copy in queue[:READ_AHEAD]:
        copy.start()
    taken = [0]

    def arrive(count):
        for index in range(taken[0], taken[0] + count):
            queue[index].wait()
            if index + READ_AHEAD < len(queue):
                queue[index + READ_AHEAD].start()
        taken[0] += count

    squares = jnp.zeros((rows, width), F32)
    for j in range(blocks):
        wide = tokens_ref[j].astype(F32)
        squares = squares + wide * wide
        scaled_ref[:, j * width : (j + 1) * width] = (wide * gain_ref[j : j + 1]).astype(BF16)
    mean = jnp.sum(squares, axis=1, keepdims=True) / (blocks * width)
    inverse = lax.rsqrt(mean + EPS)
    scaled = scaled_ref[...]
    small = jnp.concatenate([beta_ref[...], decay_ref[...]], axis=0)
    raw = dot_t(scaled, small) * inverse
    every = beta_ref.shape[0]
    lane = lax.broadcasted_iota(jnp.int32, raw.shape, 1)
    first = core_ref[0] * heads

    def column(index):
        picked = jnp.sum(jnp.where(lane == first + index, raw, 0.0), axis=1, keepdims=True)
        return jnp.broadcast_to(picked, (rows, size))

    def project(index):
        raw = jnp.dot(scaled, held_ref[index], preferred_element_type=F32) * inverse
        return [raw[:, h * size : (h + 1) * size] for h in range(heads)]

    row = lax.broadcasted_iota(jnp.int32, (rows, rows), 0)
    col = lax.broadcasted_iota(jnp.int32, (rows, rows), 1)
    same = row // steps == col // steps
    all_heads = range(heads)
    lanes = [slice(h * size, (h + 1) * size) for h in all_heads]
    rates, totals = [], []
    for h in all_heads:
        rates.append(1.0 / (1.0 + jnp.exp(-column(h))))
        lift = column(every + h)
        soft = jnp.maximum(lift, 0.0) + jnp.log1p(jnp.exp(-jnp.abs(lift)))
        totals.append(chain_terms(-jnp.exp(log_ref[:, h : h + 1]) * soft, steps)[0])
    arrive(CUTS)
    keys = [unit(silu(raw)) for raw in project(1)]
    mixes, fades = zip(*(chain_mix(keys[h], rates[h], totals[h], steps) for h in all_heads))
    arrive(CUTS)
    queries = [unit(silu(raw)) * size ** (-0.5) for raw in project(0)]
    weights = [fades[h] * dot_t(queries[h], keys[h]) for h in all_heads]

    def caught_up(left, h):
        recent = jnp.where(same, dot_t(left, unit_ref[:, lanes[h]]), 0.0)
        return dot(recent, writes_ref[:, lanes[h]])

    recents = [(caught_up(keys[h], h), caught_up(queries[h], h)) for h in all_heads]
    arrive(heads)
    recalls, seens = [], []
    for h in all_heads:
        recalled, seen = by_sequence([keys[h], queries[h]], lambda s: near_ref[h, s], steps)
        whole = whole_ref[:, lanes[h]]
        decay = jnp.exp(totals[h])
        recalls.append(rates[h] * decay * (whole * recalled + recents[h][0]))
        seens.append(decay * (whole * seen + recents[h][1]))
    arrive(CUTS)
    reads = []
    for h, raw in enumerate(project(2)):
        writes = chain_writes(mixes[h], rates[h] * silu(raw) - recalls[h])
        value = seens[h] + dot(weights[h], writes)
        mean = jnp.sum(value * value, axis=1, keepdims=True) / size
        reads.append(value * lax.rsqrt(mean + EPS) * head_gain_ref[...])
    arrive(CUTS)
    for h, raw in enumerate(project(3)):
        out_ref[:, lanes[h]] = (reads[h] * silu(raw)).astype(BF16)


def read(core, tokens, gain, weights, beta, decay, decay_log, head_gain, state, kept, steps):
    blocks, rows, width = tokens.shape
    heads, _, size, _ = state.shape
    return pl.pallas_call(
        functools.partial(read_kernel, steps),
        out_shape=VMEM((rows, heads * size), BF16),
        in_specs=[SCALAR] + [WHOLE] * 2 + [FAR] * 4 + [WHOLE] * 4 + [FAR] + [WHOLE] * 3,
        out_specs=WHOLE,
        scratch_shapes=[
            pltpu.VMEM((rows, blocks * width), BF16),
            pltpu.VMEM((4, blocks * width, heads * size), BF16),
            pltpu.VMEM(state.shape, BF16),
            pltpu.SemaphoreType.DMA((4 * CUTS,)),
            pltpu.SemaphoreType.DMA((heads,)),
        ],
        compiler_params=params(24),
        name="read",
    )(core, tokens, gain, *weights, beta, decay, decay_log, head_gain, state, *kept)


def project_kernel(team, *refs):
    *weight_refs, full_ref, send_ref = refs[team:]
    rows = jnp.concatenate([ref[...] for ref in refs[:team]], axis=0)
    for a in range(team):
        for y in range(Y):
            value = dot_t(weight_refs[y][a], rows)
            full_ref[a * Y + y] = value
            send_ref[a * Y + y] = value.astype(BF16)


def project(parts, weights):
    pairs, cols, _ = weights[0].shape
    shape = (pairs * len(weights), cols, len(parts) * parts[0].shape[0])
    return pl.pallas_call(
        functools.partial(project_kernel, len(parts)),
        out_shape=(VMEM(shape, F32), VMEM(shape, BF16)),
        in_specs=[WHOLE] * (len(parts) + len(weights)),
        out_specs=(WHOLE,) * 2,
        compiler_params=params(8),
        name="project",
    )(*parts, *weights)


def combine_kernel(core_ref, mine_ref, other_ref, sum_ref, square_ref):
    blocks, cols, rows = mine_ref.shape
    half = cols // 2
    squares = jnp.zeros((8, rows), F32)
    for j in range(blocks):
        value = mine_ref[j] + other_ref[j].astype(F32)
        squares = squares + jnp.sum((value * value).reshape(cols // 8, 8, rows), axis=0)
    square_ref[...] = squares
    own = pl.ds(pl.multiple_of(core_ref[0] * half, half), half)
    for j in range(blocks):
        sum_ref[j] = mine_ref[j, own, :] + other_ref[j, own, :].astype(F32)


def combine(core, mine, other):
    blocks, cols, rows = mine.shape
    return pl.pallas_call(
        combine_kernel,
        out_shape=(VMEM((blocks, cols // 2, rows), F32), VMEM((8, rows), F32)),
        in_specs=[SCALAR, WHOLE, WHOLE],
        out_specs=(WHOLE,) * 2,
        compiler_params=params(8),
        name="combine",
    )(core, mine, other)


def normalize_kernel(team, model, place_ref, sum_ref, *refs):
    out_ref = refs[team]
    blocks, _, rows = sum_ref.shape
    span = rows // team
    factors = []
    for e in range(team):
        total = 0.0
        for f in range(team):
            part = refs[f][:, (e ^ f) * span : ((e ^ f) + 1) * span]
            total = total + jnp.sum(part, axis=0, keepdims=True)
        factors.append(lax.rsqrt(total / model + EPS))
    factor = jnp.concatenate(factors, axis=1)
    for j in range(blocks):
        out_ref[jnp.bitwise_xor(place_ref[0], j)] = (sum_ref[j] * factor).astype(BF16)


def normalize(place, sums, squares, model):
    return pl.pallas_call(
        functools.partial(normalize_kernel, len(squares), model),
        out_shape=VMEM(sums.shape, BF16),
        in_specs=[SCALAR] + [WHOLE] * (1 + len(squares)),
        out_specs=WHOLE,
        compiler_params=params(8),
        name="normalize",
    )(place, sums, *squares)


def spread_kernel(team, depth_ref, value_ref, gain_ref, out_ref):
    blocks, _, rows = value_ref.shape
    span = rows // team
    gain = gain_ref[...]
    depth = depth_ref[0]
    for m in range(blocks):
        sender = (m // Y) * team + depth % team if team < Y else depth
        value = value_ref[m].astype(F32) * gain
        for e in range(team):
            source = jnp.bitwise_xor(sender, e) * Y + m % Y
            lanes = pl.ds(pl.multiple_of(source * span, span), span)
            out_ref[:, lanes] = value[:, e * span : (e + 1) * span].astype(BF16)


def spread(depth, value, gain, team):
    blocks, cols, rows = value.shape
    return pl.pallas_call(
        functools.partial(spread_kernel, team),
        out_shape=jax.ShapeDtypeStruct((cols, blocks * rows), BF16),
        in_specs=[SCALAR, WHOLE, WHOLE],
        compiler_params=params(8),
        name="spread",
    )(depth, value, gain)


def layer(
    tokens,
    pre_gain,
    query_weight,
    key_weight,
    value_weight,
    gate_weight,
    beta_weight,
    decay_weight,
    decay_log,
    head_gain,
    out_weight,
    post_gain,
    saved_state,
    earlier_keys,
    earlier_values,
    earlier_rates,
    earlier_decays,
    accepted,
):
    seqs, heads, size, _ = saved_state.shape
    steps = earlier_keys.shape[1]
    rows = seqs * steps
    model = pre_gain.shape[0]
    groups = lax.axis_size("kv")
    deep = groups // Y
    core = lax.axis_index("tp").reshape(1)
    depth = (lax.axis_index("kv") // Y).reshape(1)
    place = (depth // TEAM) * Y + lax.axis_index("kv") % Y
    swap = [(0, 1), (1, 0)]
    members = [
        [z * Y + y for z in range(first, deep, TEAM) for y in range(Y)] for first in range(TEAM)
    ]

    def shift(value, mask):
        return lax.ppermute(value, "kv", [(k, k ^ mask) for k in range(groups)])

    flipped = out_weight.T
    across = shift(flipped, TEAM * Y)
    own = lax.all_to_all(
        tokens.reshape(groups, rows, tokens.shape[1]), "kv", 0, 0, tiled=True
    )
    two = jnp.stack([flipped, across])
    wide = []
    for y in range(1, Y):
        wide.append(near(shift(two, y)))
    state, *kept = recall(
        far(saved_state),
        far(earlier_keys),
        far(earlier_values),
        far(earlier_rates.transpose(1, 2, 0)),
        far(earlier_decays.transpose(1, 2, 0)),
        far(accepted.reshape(1, seqs)),
        steps,
    )
    state = far(state)
    kept = tuple(near(value) for value in kept)
    attended = read(
        core,
        near(own),
        near(pre_gain.reshape(groups, -1)),
        tuple(far(w) for w in (query_weight, key_weight, value_weight, gate_weight)),
        near(beta_weight.T),
        near(decay_weight.T),
        near(decay_log.reshape(1, heads)),
        near(head_gain.reshape(1, size)),
        state,
        kept,
        steps,
    )
    parts = [attended] + [shift(attended, e * Y) for e in range(1, TEAM)]
    full, send = project([near(part) for part in parts], [near(two), *wide])
    other = lax.ppermute(send, "tp", swap)
    sums, squares = combine(core, near(full), near(other))
    squares = [squares] + [shift(squares, e * Y) for e in range(1, TEAM)]
    packed = normalize(place, near(sums), [near(part) for part in squares], model)
    arrived = lax.all_to_all(packed, "kv", 0, 0, axis_index_groups=members, tiled=True)
    committed = commit(far(saved_state), *kept, steps)
    mixed = spread(depth, near(arrived), near(post_gain.reshape(-1, 1)), TEAM).T
    return (mixed, committed)


def solution(mesh):
    placed = (
        P("dp", "kv"),
        P(),
        P(None, "tp"),
        P(None, "tp"),
        P(None, "tp"),
        P(None, "tp"),
        P(),
        P(),
        P("tp"),
        P(),
        P("tp", "kv"),
        P(("kv", "tp")),
        P(("dp", "kv"), "tp", None, None),
        P(("dp", "kv"), None, "tp", None),
        P(("dp", "kv"), None, "tp", None),
        P(("dp", "kv"), None, "tp"),
        P(("dp", "kv"), None, "tp"),
        P(("dp", "kv")),
    )
    return jax.shard_map(
        layer,
        mesh=mesh,
        in_specs=placed,
        out_specs=(P("dp", ("kv", "tp")), P(("dp", "kv"), "tp", None, None)),
        check_vma=False,
    )
```

```python
import functools
import jax
import jax.numpy as jnp
from jax import lax
from jax.experimental import pallas as pl
from jax.experimental.pallas import tpu as pltpu
from jax.sharding import PartitionSpec as P

F32 = jnp.float32
BF16 = jnp.bfloat16
EPS = 1e-06
AHEAD = 4
READ_AHEAD = 6
CUTS = 2
Y = 4
TEAM = 2
VMEM = pltpu.VMEM
WHOLE = pl.BlockSpec(memory_space=pltpu.VMEM)
FAR = pl.BlockSpec(memory_space=pltpu.HBM)
SCALAR = pl.BlockSpec(memory_space=pltpu.SMEM)


def params(mib):
    return pltpu.CompilerParams(vmem_limit_bytes=mib * 1024 * 1024)


def near(value):
    return pltpu.with_memory_space_constraint(value, pltpu.VMEM)


def far(value):
    return pltpu.with_memory_space_constraint(value, pltpu.HBM)


def dot(a, b):
    return jnp.dot(a.astype(BF16), b.astype(BF16), preferred_element_type=F32)


def dot_t(a, b):
    return lax.dot_general(
        a.astype(BF16), b.astype(BF16), (((1,), (1,)), ((), ())), preferred_element_type=F32
    )


def unit(values):
    return values * lax.rsqrt(jnp.sum(values * values, axis=-1, keepdims=True) + EPS)


def silu(values):
    return values / (1.0 + jnp.exp(-values))


def chain_terms(log_decays, steps):
    rows = log_decays.shape[0]
    place = lax.broadcasted_iota(jnp.int32, log_decays.shape, 0) % steps
    total = log_decays
    shift = 1
    while shift < steps:
        total = total + jnp.where(place >= shift, pltpu.roll(total, shift, 0), 0.0)
        shift *= 2
    rest = jnp.where(place + 1 < steps, pltpu.roll(log_decays, rows - 1, 0), 0.0)
    shift = 1
    while shift < steps:
        rest = rest + jnp.where(place + shift < steps, pltpu.roll(rest, rows - shift, 0), 0.0)
        shift *= 2
    return total, rest


def chain_mix(keys, rates, total, steps):
    rows = keys.shape[0]
    row = lax.broadcasted_iota(jnp.int32, (rows, rows), 0)
    col = lax.broadcasted_iota(jnp.int32, (rows, rows), 1)
    upto = (row // steps == col // steps) & (col <= row)
    fade = jnp.exp(jnp.where(upto, total - total.T, 0.0))
    mix = jnp.where(upto & (col < row), rates * fade * dot_t(keys, keys), 0.0)
    return mix.astype(BF16), jnp.where(upto, fade, 0.0)


def chain_writes(mix, start):
    done = start + dot(mix, dot(mix, start))
    return done - dot(mix, done)


def by_sequence(left, states, steps):
    rows = left[0].shape[0]
    tile = 8
    per = tile // steps
    outs = [[] for _ in left]
    for first in range(0, rows, tile):
        stack = jnp.concatenate([part[first : first + tile] for part in left], axis=0)
        held = jnp.concatenate([states(first // steps + i) for i in range(per)], axis=1)
        size = held.shape[1] // per
        got = dot(stack, held)
        which = lax.broadcasted_iota(jnp.int32, (tile, size), 0) // steps
        for index in range(len(left)):
            piece = got[index * tile : (index + 1) * tile]
            value = piece[:, :size]
            for i in range(1, per):
                value = jnp.where(which == i, piece[:, i * size : (i + 1) * size], value)
            outs[index].append(value)
    return [jnp.concatenate(part, axis=0) for part in outs]


def recall_kernel(
    steps,
    source_ref,
    keys_ref,
    values_ref,
    rates_ref,
    decays_ref,
    accepted_ref,
    state_ref,
    unit_ref,
    writes_ref,
    whole_ref,
    held_ref,
    short_ref,
    flat_ref,
    given_ref,
    chain_ref,
    count_ref,
    small_sems,
    in_sems,
    out_sems,
):
    heads, seqs, size, _ = held_ref.shape
    rows = seqs * steps
    arrive = [
        pltpu.make_async_copy(source_ref.at[:, h], held_ref.at[h], in_sems.at[h])
        for h in range(heads)
    ]
    leave = [
        pltpu.make_async_copy(short_ref.at[h], state_ref.at[h], out_sems.at[h])
        for h in range(heads)
    ]
    small = [
        pltpu.make_async_copy(keys_ref, given_ref.at[0], small_sems.at[0]),
        pltpu.make_async_copy(values_ref, given_ref.at[1], small_sems.at[1]),
        pltpu.make_async_copy(rates_ref, chain_ref.at[0], small_sems.at[2]),
        pltpu.make_async_copy(decays_ref, chain_ref.at[1], small_sems.at[3]),
        pltpu.make_async_copy(accepted_ref, count_ref, small_sems.at[4]),
    ]
    for copy in small + arrive[:AHEAD]:
        copy.start()
    for copy in small:
        copy.wait()
    table = jnp.concatenate(
        [chain_ref[i, p] for i in range(2) for p in range(steps)]
        + [jnp.broadcast_to(count_ref[...].astype(F32), (8, seqs))],
        axis=0,
    )
    pick = (
        lax.broadcasted_iota(jnp.int32, (rows, seqs), 0) // steps
        == lax.broadcasted_iota(jnp.int32, (rows, seqs), 1)
    ).astype(F32)
    spread = lax.dot_general(
        pick,
        table,
        (((1,), (1,)), ((), ())),
        precision=lax.Precision.HIGHEST,
        preferred_element_type=F32,
    )
    lane = lax.broadcasted_iota(jnp.int32, spread.shape, 1)
    place = lax.broadcasted_iota(jnp.int32, spread.shape, 0) % steps
    count = steps * heads

    def column(index):
        picked = jnp.sum(jnp.where(lane == index, spread, 0.0), axis=1, keepdims=True)
        return jnp.broadcast_to(picked, (rows, size))

    live = column(2 * count) > place[:, :1].astype(F32)

    def own(first):
        return jnp.where(live, column(first + place * heads), 0.0)

    for i in range(2):
        flat_ref[i] = given_ref[i].astype(F32).reshape(rows * heads, size)
    ready = []
    for h in range(heads):
        lanes = slice(h * size, (h + 1) * size)
        keys = unit(flat_ref[0, pl.ds(h, rows, heads), :])
        rates = own(h)
        total, rest = chain_terms(own(count + h), steps)
        mix, _ = chain_mix(keys, rates, total, steps)
        unit_ref[:, lanes] = keys.astype(BF16)
        whole_ref[:, lanes] = jnp.exp(total + rest)
        given = rates * flat_ref[1, pl.ds(h, rows, heads), :]
        ready.append((keys, mix, given, rates * jnp.exp(total), jnp.exp(rest)))
    starts = []
    for h in range(heads):
        keys, mix, given, scale, _ = ready[h]
        arrive[h].wait()
        if h + AHEAD < heads:
            arrive[h + AHEAD].start()
        short_ref[h] = held_ref[h].astype(BF16)
        leave[h].start()
        (recalled,) = by_sequence([keys], lambda s: short_ref[h, s], steps)
        starts.append(given - scale * recalled)
    for h in range(heads):
        lanes = slice(h * size, (h + 1) * size)
        writes_ref[:, lanes] = (ready[h][4] * chain_writes(ready[h][1], starts[h])).astype(BF16)
    for copy in leave:
        copy.wait()


def recall(state, keys, values, rates, decays, accepted, steps):
    seqs, heads, size, _ = state.shape
    rows, width = seqs * steps, heads * size
    turned = (heads, seqs, size, size)
    return pl.pallas_call(
        functools.partial(recall_kernel, steps),
        out_shape=(
            pltpu.HBM(turned, BF16),
            VMEM((rows, width), BF16),
            VMEM((rows, width), BF16),
            VMEM((rows, width), F32),
        ),
        in_specs=[FAR] * 6,
        out_specs=(FAR,) + (WHOLE,) * 3,
        scratch_shapes=[
            pltpu.VMEM(turned, F32),
            pltpu.VMEM(turned, BF16),
            pltpu.VMEM((2, rows * heads, size), F32),
            pltpu.VMEM((2, *keys.shape), BF16),
            pltpu.VMEM((2, *rates.shape), F32),
            pltpu.VMEM(accepted.shape, jnp.int32),
            pltpu.SemaphoreType.DMA((5,)),
            pltpu.SemaphoreType.DMA((heads,)),
            pltpu.SemaphoreType.DMA((heads,)),
        ],
        compiler_params=params(20),
        name="recall",
    )(state, keys, values, rates, decays, accepted)


COMMIT_BLOCK = 4
COMMIT_AHEAD = 3


def commit_kernel(steps, state_ref, unit_ref, writes_ref, whole_ref, out_ref, held_ref, ins, outs):
    seqs, heads, size, _ = held_ref.shape
    span = COMMIT_BLOCK * steps

    def part(ref, step):
        return ref.at[pl.ds(step * COMMIT_BLOCK, COMMIT_BLOCK)]

    def arrive(step):
        return pltpu.make_async_copy(part(state_ref, step), part(held_ref, step), ins.at[step])

    def leave(step):
        return pltpu.make_async_copy(part(held_ref, step), part(out_ref, step), outs.at[step])

    count = seqs // COMMIT_BLOCK
    for step in range(COMMIT_AHEAD):
        arrive(step).start()
    group = lax.broadcasted_iota(jnp.int32, (span, size), 0) // steps

    def body(step, carry):
        base = pl.multiple_of(step * span, span)
        arrive(step).wait()

        @pl.when(step + COMMIT_AHEAD < count)
        def _():
            arrive(step + COMMIT_AHEAD).start()

        for h in range(heads):
            lanes = slice(h * size, (h + 1) * size)
            keys_t = unit_ref[pl.ds(base, span), lanes].astype(F32).T.astype(BF16)
            writes = writes_ref[pl.ds(base, span), lanes].astype(F32)
            whole = whole_ref[pl.ds(base, span), lanes]
            for s in range(0, COMMIT_BLOCK, 2):
                pair = jnp.concatenate(
                    [jnp.where(group == s + i, writes, 0.0).astype(BF16) for i in range(2)], axis=1
                )
                added = jnp.dot(keys_t, pair, preferred_element_type=F32)
                for i in range(2):
                    scale = whole[(s + i) * steps : (s + i) * steps + 1]
                    at = step * COMMIT_BLOCK + s + i
                    held_ref[at, h] = scale * held_ref[at, h] + added[:, i * size : (i + 1) * size]
        leave(step).start()
        return carry

    lax.fori_loop(0, count, body, 0)
    for step in range(count):
        leave(step).wait()


def commit(state, keys, writes, whole, steps):
    count = state.shape[0] // COMMIT_BLOCK
    return pl.pallas_call(
        functools.partial(commit_kernel, steps),
        out_shape=pltpu.HBM(state.shape, F32),
        in_specs=[FAR] + [WHOLE] * 3,
        out_specs=FAR,
        scratch_shapes=[
            pltpu.VMEM(state.shape, F32),
            pltpu.SemaphoreType.DMA((count,)),
            pltpu.SemaphoreType.DMA((count,)),
        ],
        compiler_params=params(16),
        cost_estimate=pl.CostEstimate(flops=4 * 10**9, bytes_accessed=0, transcendentals=0),
        name="commit",
    )(state, keys, writes, whole)


def read_kernel(
    steps,
    core_ref,
    tokens_ref,
    gain_ref,
    query_ref,
    key_ref,
    value_ref,
    gate_ref,
    beta_ref,
    decay_ref,
    log_ref,
    head_gain_ref,
    state_ref,
    unit_ref,
    writes_ref,
    whole_ref,
    out_ref,
    scaled_ref,
    held_ref,
    near_ref,
    sems,
    state_sems,
):
    blocks, rows, width = tokens_ref.shape
    heads, _, size, _ = state_ref.shape
    part = blocks * width // CUTS
    copies = [
        [
            pltpu.make_async_copy(
                ref.at[pl.ds(c * part, part)],
                held_ref.at[i, pl.ds(c * part, part)],
                sems.at[i * CUTS + c],
            )
            for c in range(CUTS)
        ]
        for i, ref in enumerate((query_ref, key_ref, value_ref, gate_ref))
    ]
    states = [
        pltpu.make_async_copy(state_ref.at[h], near_ref.at[h], state_sems.at[h])
        for h in range(heads)
    ]
    queue = [*copies[1], *copies[0], *states, *copies[2], *copies[3]]
    for copy in queue[:READ_AHEAD]:
        copy.start()
    taken = [0]

    def arrive(count):
        for index in range(taken[0], taken[0] + count):
            queue[index].wait()
            if index + READ_AHEAD < len(queue):
                queue[index + READ_AHEAD].start()
        taken[0] += count

    squares = jnp.zeros((rows, width), F32)
    for j in range(blocks):
        wide = tokens_ref[j].astype(F32)
        squares = squares + wide * wide
        scaled_ref[:, j * width : (j + 1) * width] = (wide * gain_ref[j : j + 1]).astype(BF16)
    mean = jnp.sum(squares, axis=1, keepdims=True) / (blocks * width)
    inverse = lax.rsqrt(mean + EPS)
    scaled = scaled_ref[...]
    small = jnp.concatenate([beta_ref[...], decay_ref[...]], axis=0)
    raw = dot_t(scaled, small) * inverse
    every = beta_ref.shape[0]
    lane = lax.broadcasted_iota(jnp.int32, raw.shape, 1)
    first = core_ref[0] * heads

    def column(index):
        picked = jnp.sum(jnp.where(lane == first + index, raw, 0.0), axis=1, keepdims=True)
        return jnp.broadcast_to(picked, (rows, size))

    def project(index):
        raw = jnp.dot(scaled, held_ref[index], preferred_element_type=F32) * inverse
        return [raw[:, h * size : (h + 1) * size] for h in range(heads)]

    row = lax.broadcasted_iota(jnp.int32, (rows, rows), 0)
    col = lax.broadcasted_iota(jnp.int32, (rows, rows), 1)
    same = row // steps == col // steps
    all_heads = range(heads)
    lanes = [slice(h * size, (h + 1) * size) for h in all_heads]
    rates, totals = [], []
    for h in all_heads:
        rates.append(1.0 / (1.0 + jnp.exp(-column(h))))
        lift = column(every + h)
        soft = jnp.maximum(lift, 0.0) + jnp.log1p(jnp.exp(-jnp.abs(lift)))
        totals.append(chain_terms(-jnp.exp(log_ref[:, h : h + 1]) * soft, steps)[0])
    arrive(CUTS)
    keys = [unit(silu(raw)) for raw in project(1)]
    mixes, fades = zip(*(chain_mix(keys[h], rates[h], totals[h], steps) for h in all_heads))
    arrive(CUTS)
    queries = [unit(silu(raw)) * size ** (-0.5) for raw in project(0)]
    weights = [fades[h] * dot_t(queries[h], keys[h]) for h in all_heads]

    def caught_up(left, h):
        recent = jnp.where(same, dot_t(left, unit_ref[:, lanes[h]]), 0.0)
        return dot(recent, writes_ref[:, lanes[h]])

    recents = [(caught_up(keys[h], h), caught_up(queries[h], h)) for h in all_heads]
    arrive(heads)
    recalls, seens = [], []
    for h in all_heads:
        recalled, seen = by_sequence([keys[h], queries[h]], lambda s: near_ref[h, s], steps)
        whole = whole_ref[:, lanes[h]]
        decay = jnp.exp(totals[h])
        recalls.append(rates[h] * decay * (whole * recalled + recents[h][0]))
        seens.append(decay * (whole * seen + recents[h][1]))
    arrive(CUTS)
    reads = []
    for h, raw in enumerate(project(2)):
        writes = chain_writes(mixes[h], rates[h] * silu(raw) - recalls[h])
        value = seens[h] + dot(weights[h], writes)
        mean = jnp.sum(value * value, axis=1, keepdims=True) / size
        reads.append(value * lax.rsqrt(mean + EPS) * head_gain_ref[...])
    arrive(CUTS)
    for h, raw in enumerate(project(3)):
        out_ref[:, lanes[h]] = (reads[h] * silu(raw)).astype(BF16)


def read(core, tokens, gain, weights, beta, decay, decay_log, head_gain, state, kept, steps):
    blocks, rows, width = tokens.shape
    heads, _, size, _ = state.shape
    return pl.pallas_call(
        functools.partial(read_kernel, steps),
        out_shape=VMEM((rows, heads * size), BF16),
        in_specs=[SCALAR] + [WHOLE] * 2 + [FAR] * 4 + [WHOLE] * 4 + [FAR] + [WHOLE] * 3,
        out_specs=WHOLE,
        scratch_shapes=[
            pltpu.VMEM((rows, blocks * width), BF16),
            pltpu.VMEM((4, blocks * width, heads * size), BF16),
            pltpu.VMEM(state.shape, BF16),
            pltpu.SemaphoreType.DMA((4 * CUTS,)),
            pltpu.SemaphoreType.DMA((heads,)),
        ],
        compiler_params=params(24),
        name="read",
    )(core, tokens, gain, *weights, beta, decay, decay_log, head_gain, state, *kept)


def project_kernel(team, *refs):
    *weight_refs, full_ref, send_ref = refs[team:]
    rows = jnp.concatenate([ref[...] for ref in refs[:team]], axis=0)
    for a in range(team):
        for y in range(Y):
            value = dot(rows, weight_refs[y][a]).T
            full_ref[a * Y + y] = value
            send_ref[a * Y + y] = value.astype(BF16)


def project(parts, weights):
    pairs, _, cols = weights[0].shape
    shape = (pairs * len(weights), cols, len(parts) * parts[0].shape[0])
    return pl.pallas_call(
        functools.partial(project_kernel, len(parts)),
        out_shape=(VMEM(shape, F32), VMEM(shape, BF16)),
        in_specs=[WHOLE] * (len(parts) + len(weights)),
        out_specs=(WHOLE,) * 2,
        compiler_params=params(8),
        name="project",
    )(*parts, *weights)


def combine_kernel(core_ref, mine_ref, other_ref, sum_ref, square_ref):
    blocks, cols, rows = mine_ref.shape
    half = cols // 2
    squares = jnp.zeros((8, rows), F32)
    for j in range(blocks):
        value = mine_ref[j] + other_ref[j].astype(F32)
        squares = squares + jnp.sum((value * value).reshape(cols // 8, 8, rows), axis=0)
    square_ref[...] = squares
    own = pl.ds(pl.multiple_of(core_ref[0] * half, half), half)
    for j in range(blocks):
        sum_ref[j] = mine_ref[j, own, :] + other_ref[j, own, :].astype(F32)


def combine(core, mine, other):
    blocks, cols, rows = mine.shape
    return pl.pallas_call(
        combine_kernel,
        out_shape=(VMEM((blocks, cols // 2, rows), F32), VMEM((8, rows), F32)),
        in_specs=[SCALAR, WHOLE, WHOLE],
        out_specs=(WHOLE,) * 2,
        compiler_params=params(8),
        name="combine",
    )(core, mine, other)


def normalize_kernel(team, model, place_ref, sum_ref, *refs):
    out_ref = refs[team]
    blocks, _, rows = sum_ref.shape
    span = rows // team
    factors = []
    for e in range(team):
        total = 0.0
        for f in range(team):
            part = refs[f][:, (e ^ f) * span : ((e ^ f) + 1) * span]
            total = total + jnp.sum(part, axis=0, keepdims=True)
        factors.append(lax.rsqrt(total / model + EPS))
    factor = jnp.concatenate(factors, axis=1)
    for j in range(blocks):
        out_ref[jnp.bitwise_xor(place_ref[0], j)] = (sum_ref[j] * factor).astype(BF16)


def normalize(place, sums, squares, model):
    return pl.pallas_call(
        functools.partial(normalize_kernel, len(squares), model),
        out_shape=VMEM(sums.shape, BF16),
        in_specs=[SCALAR] + [WHOLE] * (1 + len(squares)),
        out_specs=WHOLE,
        compiler_params=params(8),
        name="normalize",
    )(place, sums, *squares)


def spread_kernel(team, depth_ref, value_ref, gain_ref, out_ref):
    blocks, _, rows = value_ref.shape
    span = rows // team
    gain = gain_ref[...]
    depth = depth_ref[0]
    for m in range(blocks):
        sender = (m // Y) * team + depth % team if team < Y else depth
        value = value_ref[m].astype(F32) * gain
        for e in range(team):
            source = jnp.bitwise_xor(sender, e) * Y + m % Y
            lanes = pl.ds(pl.multiple_of(source * span, span), span)
            out_ref[:, lanes] = value[:, e * span : (e + 1) * span].astype(BF16)


def spread(depth, value, gain, team):
    blocks, cols, rows = value.shape
    return pl.pallas_call(
        functools.partial(spread_kernel, team),
        out_shape=jax.ShapeDtypeStruct((cols, blocks * rows), BF16),
        in_specs=[SCALAR, WHOLE, WHOLE],
        compiler_params=params(8),
        name="spread",
    )(depth, value, gain)


def layer(
    tokens,
    pre_gain,
    query_weight,
    key_weight,
    value_weight,
    gate_weight,
    beta_weight,
    decay_weight,
    decay_log,
    head_gain,
    out_weight,
    post_gain,
    saved_state,
    earlier_keys,
    earlier_values,
    earlier_rates,
    earlier_decays,
    accepted,
):
    seqs, heads, size, _ = saved_state.shape
    steps = earlier_keys.shape[1]
    rows = seqs * steps
    model = pre_gain.shape[0]
    groups = lax.axis_size("kv")
    deep = groups // Y
    core = lax.axis_index("tp").reshape(1)
    depth = (lax.axis_index("kv") // Y).reshape(1)
    place = (depth // TEAM) * Y + lax.axis_index("kv") % Y
    swap = [(0, 1), (1, 0)]
    members = [
        [z * Y + y for z in range(first, deep, TEAM) for y in range(Y)] for first in range(TEAM)
    ]

    def shift(value, mask):
        return lax.ppermute(value, "kv", [(k, k ^ mask) for k in range(groups)])

    flipped = out_weight
    across = shift(flipped, TEAM * Y)
    own = lax.all_to_all(
        tokens.reshape(groups, rows, tokens.shape[1]), "kv", 0, 0, tiled=True
    )
    two = jnp.stack([flipped, across])
    wide = []
    for y in range(1, Y):
        wide.append(near(shift(two, y)))
    state, *kept = recall(
        far(saved_state),
        far(earlier_keys),
        far(earlier_values),
        far(earlier_rates.transpose(1, 2, 0)),
        far(earlier_decays.transpose(1, 2, 0)),
        far(accepted.reshape(1, seqs)),
        steps,
    )
    state = far(state)
    kept = tuple(near(value) for value in kept)
    attended = read(
        core,
        near(own),
        near(pre_gain.reshape(groups, -1)),
        tuple(far(w) for w in (query_weight, key_weight, value_weight, gate_weight)),
        near(beta_weight.T),
        near(decay_weight.T),
        near(decay_log.reshape(1, heads)),
        near(head_gain.reshape(1, size)),
        state,
        kept,
        steps,
    )
    parts = [attended] + [shift(attended, e * Y) for e in range(1, TEAM)]
    full, send = project([near(part) for part in parts], [near(two), *wide])
    other = lax.ppermute(send, "tp", swap)
    sums, squares = combine(core, near(full), near(other))
    squares = [squares] + [shift(squares, e * Y) for e in range(1, TEAM)]
    packed = normalize(place, near(sums), [near(part) for part in squares], model)
    arrived = lax.all_to_all(packed, "kv", 0, 0, axis_index_groups=members, tiled=True)
    committed = commit(far(saved_state), *kept, steps)
    mixed = spread(depth, near(arrived), near(post_gain.reshape(-1, 1)), TEAM).T
    return (mixed, committed)


def solution(mesh):
    placed = (
        P("dp", "kv"),
        P(),
        P(None, "tp"),
        P(None, "tp"),
        P(None, "tp"),
        P(None, "tp"),
        P(),
        P(),
        P("tp"),
        P(),
        P("tp", "kv"),
        P(("kv", "tp")),
        P(("dp", "kv"), "tp", None, None),
        P(("dp", "kv"), None, "tp", None),
        P(("dp", "kv"), None, "tp", None),
        P(("dp", "kv"), None, "tp"),
        P(("dp", "kv"), None, "tp"),
        P(("dp", "kv")),
    )
    return jax.shard_map(
        layer,
        mesh=mesh,
        in_specs=placed,
        out_specs=(P("dp", ("kv", "tp")), P(("dp", "kv"), "tp", None, None)),
        check_vma=False,
    )
```
